32 devices in a mesh: sp: 4 (over z), fs: 4 (over y, x), tp: 2 (over core).
Axes of the slice: x: 2, y: 2, z: 4, core: 2. Of those that a mesh axis runs over, the one named last changes fastest.
Arguments:
- tokens: bfloat16 [1024, 2048], P('sp'), may hold values from -6 to 6
- norm_gain: float32 [2048], replicated, may hold values from 0.1 to 1.9
- conv_value: bfloat16 [2048, 1024], P('sp', ('fs', 'tp')), may hold values from -0.125 to 0.125
- conv_gate: bfloat16 [2048, 1024], P('sp', ('fs', 'tp')), may hold values from -0.125 to 0.125
- mixer_gate: bfloat16 [2048, 1024], P('sp', ('fs', 'tp')), may hold values from -0.125 to 0.125
- state_input: bfloat16 [2048, 1024], P('sp', ('fs', 'tp')), may hold values from -0.125 to 0.125
- write_projection: bfloat16 [2048, 1024], P('sp', ('fs', 'tp')), may hold values from -0.125 to 0.125
- state_read: bfloat16 [2048, 1024], P('sp', ('fs', 'tp')), may hold values from -0.125 to 0.125
- step_proj: bfloat16 [2048, 16], replicated, may hold values from -0.125 to 0.125
- step_bias: float32 [16], P(('fs', 'tp')), may hold values from -6 to -0.5
- decay_log: float32 [16], P(('fs', 'tp')), may hold values from -9 to -1.5
- decay_extra: float32 [16, 1024], P(('fs', 'tp'), 'sp'), may hold values from -0.8 to 0
- input_taps: float32 [4, 1024], P(None, ('fs', 'tp')), may hold values from -3 to 3
- write_taps: float32 [4, 1024], P(None, ('fs', 'tp')), may hold values from -3 to 3
- fetch_kernel_coefficients: float32 [4, 1024], P(None, ('fs', 'tp')), may hold values from -3 to 3
- long_taps: float32 [31, 1024], P(None, ('fs', 'tp')), may hold values from -5 to 5
- conv_gain: float32 [1024], P(('fs', 'tp')), may hold values from 0.1 to 1.9
- state_gain: float32 [1024], P(('fs', 'tp')), may hold values from 0.1 to 1.9
- conv_output: bfloat16 [2048, 1024], P('sp', ('fs', 'tp')), may hold values from -0.125 to 0.125
- state_output: bfloat16 [2048, 1024], P('sp', ('fs', 'tp')), may hold values from -0.125 to 0.125
- initial_state: float32 [16, 64, 128], P(('fs', 'tp')), may hold values from -12 to 12
Outputs:
- mixed: bfloat16 [1024, 2048], P(('sp', 'fs', 'tp'))
The draws below stay inside these ranges and needn't reach their ends.
All inputs are finite; a program needn't handle non-finite values.
Results may differ from the reference program's by a relative error of at most 0.017.
Values may be sent and summed in bfloat16 or wider, within the bound.
A program may use at most 64 MiB of HBM per device.

```python
import math
import jax
import jax.numpy as jnp
from jax import lax

D = 2048
C_CH = 1024
HEADS = 16
HEAD_P = 64
GROUPS = 8
STATE = 128
WIDE_TAPS = 31
SHORT_TAPS = 4
SPAN = 64
TOK_DEV = 256
D_INNER = 1024
SEQ = 1024
N_FS = 4
N_TP = 2


def head_kinds(key):
    draw = jax.random.uniform(jax.random.fold_in(key, 101), (HEADS,))
    return draw < 0.5


def draw_step_bias(key, part):
    fast = head_kinds(key)
    jitter = jax.random.uniform(jax.random.fold_in(key, 102), (HEADS,), minval=-0.5, maxval=0.5)
    slow_level = math.log(1.75) - 0.5 * math.log(SEQ)
    return (jnp.where(fast, -1.0, slow_level) + jitter).astype(jnp.float32)


def draw_decay_log(key, part):
    fast = head_kinds(key)
    jitter = jax.random.uniform(jax.random.fold_in(key, 103), (HEADS,), minval=-0.5, maxval=0.5)
    slow_level = math.log(0.114) - 0.5 * math.log(SEQ)
    return (jnp.where(fast, -2.2, slow_level) + jitter).astype(jnp.float32)


def draw_decay_extra(key, part):
    blocks = SEQ // TOK_DEV
    low, high = (math.log(0.5), math.log(2.0))
    level = jnp.exp(jax.random.uniform(jax.random.fold_in(key, 104), (HEADS, blocks), minval=low, maxval=high))
    gradual_fraction = -0.5 / SEQ * jnp.repeat(level, TOK_DEV, axis=1)
    point_locations = jax.random.randint(jax.random.fold_in(key, 105), (HEADS, 3), 0, SEQ)
    discarded_entries = jnp.log(jax.random.uniform(jax.random.fold_in(key, 106), (HEADS, 3), minval=0.5, maxval=0.8))
    location_numbers = jnp.arange(SEQ, dtype=jnp.int32)
    cluster_sets = jnp.sum(jnp.where(location_numbers[None, None, :] == point_locations[:, :, None], discarded_entries[:, :, None], 0.0), axis=1)
    return (gradual_fraction + cluster_sets).astype(jnp.float32)


def draw_long_taps(key, part):
    base = jax.random.truncated_normal(jax.random.fold_in(key, 107), -3.0, 3.0, (WIDE_TAPS, C_CH))
    ramp = math.log(3.0) * jnp.arange(C_CH, dtype=jnp.float32) / C_CH
    ramp = ramp + jax.random.uniform(jax.random.fold_in(key, 108), (C_CH,), minval=-0.35, maxval=0.35)
    return (base * jnp.exp(ramp)[None, :] / math.sqrt(WIDE_TAPS)).astype(jnp.float32)


def levels(stream_key, shape, cuts, least, top_value):
    loudness = 1.0
    for axis_at, blocks in cuts:
        heights = jax.random.uniform(jax.random.fold_in(jax.random.fold_in(stream_key, 6), axis_at), (blocks,), jnp.float32, least / len(cuts), top_value / len(cuts))
        loudness = loudness * jnp.repeat(jnp.exp(heights), shape[axis_at] // blocks).reshape((-1,) + (1,) * (len(shape) - 1 - axis_at))
    return loudness


def noise(own_key, shape, scale, most, shards=(), held_as=jnp.bfloat16):
    drawn = scale * jax.random.normal(own_key, shape, jnp.float32)
    if shards:
        drawn = drawn * levels(own_key, shape, shards, -0.22, 0.18)
    return jnp.clip(drawn, -most, most).astype(held_as)


def setup_inputs(seed: int = 0) -> dict:
    keys = jax.random.split(jax.random.key(seed), 22)
    return {
        "tokens": noise(keys[0], (SEQ, D), 1.0, 6.0, ((0, 4),)),
        "norm_gain": jnp.clip(1.0 + 0.18 * jax.random.normal(keys[1], (D,), jnp.float32), 0.1, 1.9),
        "conv_value": noise(keys[2], (D, C_CH), D ** -0.5, 0.125, ((0, 4), (1, 8))),
        "conv_gate": noise(keys[3], (D, C_CH), D ** -0.5, 0.125, ((0, 4), (1, 8))),
        "mixer_gate": noise(keys[4], (D, D_INNER), D ** -0.5, 0.125, ((0, 4), (1, 8))),
        "state_input": noise(keys[5], (D, D_INNER), D ** -0.5, 0.125, ((0, 4), (1, 8))),
        "write_projection": noise(keys[6], (D, GROUPS * STATE), D ** -0.5, 0.125, ((0, 4), (1, 8))),
        "state_read": noise(keys[7], (D, GROUPS * STATE), D ** -0.5, 0.125, ((0, 4), (1, 8))),
        "step_proj": noise(keys[8], (D, HEADS), D ** -0.5, 0.125),
        "step_bias": draw_step_bias(jax.random.fold_in(keys[21], 71), 0),
        "decay_log": draw_decay_log(jax.random.fold_in(keys[21], 71), 0),
        "decay_extra": draw_decay_extra(jax.random.fold_in(keys[21], 71), 0),
        "input_taps": noise(keys[12], (SHORT_TAPS, D_INNER), SHORT_TAPS ** -0.5, 3.0, ((1, 8),), jnp.float32),
        "write_taps": noise(keys[13], (SHORT_TAPS, GROUPS * STATE), SHORT_TAPS ** -0.5, 3.0, ((1, 8),), jnp.float32),
        "fetch_kernel_coefficients": noise(keys[14], (SHORT_TAPS, GROUPS * STATE), SHORT_TAPS ** -0.5, 3.0, ((1, 8),), jnp.float32),
        "long_taps": draw_long_taps(jax.random.fold_in(keys[21], 71), 0),
        "conv_gain": jnp.clip(1.0 + 0.18 * jax.random.normal(keys[16], (C_CH,), jnp.float32), 0.1, 1.9),
        "state_gain": jnp.clip(1.0 + 0.18 * jax.random.normal(keys[17], (D_INNER,), jnp.float32), 0.1, 1.9),
        "conv_output": noise(keys[18], (D, C_CH), (C_CH + D_INNER) ** -0.5, 0.125, ((0, 4), (1, 8))),
        "state_output": noise(keys[19], (D, D_INNER), (C_CH + D_INNER) ** -0.5, 0.125, ((0, 4), (1, 8))),
        "initial_state": noise(keys[20], (HEADS, HEAD_P, STATE), 2.0, 12.0, ((0, 8),), jnp.float32),
    }


eps_norm = 1e-06

def causal_valid(padded, taps):
    result = lax.conv_general_dilated(padded[None], taps[:, None, :], window_strides=(1,), padding='VALID', dimension_numbers=('NWC', 'WIO', 'NWC'), feature_group_count=taps.shape[1], precision=lax.Precision.HIGHEST)
    return result[0]

def causal_conv(signal, taps):
    padded = jnp.pad(signal, ((taps.shape[0] - 1, 0), (0, 0)))
    return causal_valid(padded, taps)

def project(normed, weight):
    return jnp.dot(normed, weight, preferred_element_type=jnp.float32).astype(jnp.bfloat16)

def span_step(state, inputs):
    x_span, write_span, read_span, log_span = inputs
    cumul = jnp.cumsum(log_span, axis=0)
    length = cumul.shape[0]
    lower = jnp.tril(jnp.ones((length, length), dtype=bool))
    gaps = cumul.T[:, :, None] - cumul.T[:, None, :]
    weights = jnp.where(lower, jnp.exp(jnp.where(lower, gaps, 0.0)), 0.0)
    scores = jnp.einsum('thn,shn->hts', read_span, write_span, precision=lax.Precision.HIGHEST)
    inner = jnp.einsum('hts,shp->thp', scores * weights, x_span, precision=lax.Precision.HIGHEST)
    carried = jnp.einsum('thn,hpn->thp', read_span, state, precision=lax.Precision.HIGHEST) * jnp.exp(cumul)[:, :, None]
    last = cumul[-1]
    fresh = jnp.einsum('shn,shp->hpn', write_span * jnp.exp(last[None, :] - cumul)[:, :, None], x_span, precision=lax.Precision.HIGHEST)
    return (state * jnp.exp(last)[:, None, None] + fresh, inner + carried)

def reference(tokens, norm_gain, conv_value, conv_gate, mixer_gate, state_input, write_projection, state_read, step_proj, step_bias, decay_log, decay_extra, input_taps, write_taps, fetch_kernel_coefficients, long_taps, conv_gain, state_gain, conv_output, state_output, initial_state):
    length = tokens.shape[0]
    values = tokens.astype(jnp.float32)
    normed = (values * lax.rsqrt(lax.optimization_barrier(jnp.mean(values * values, axis=1, keepdims=True)) + eps_norm) * norm_gain).astype(jnp.bfloat16)
    value_rows = project(normed, conv_value)
    gate_rows = project(normed, conv_gate)
    gate_z = project(normed, mixer_gate)
    input_rows = project(normed, state_input)
    write_rows = project(normed, write_projection)
    read_rows = project(normed, state_read)
    step_size = jax.nn.softplus(jnp.dot(normed, step_proj, preferred_element_type=jnp.float32) + step_bias)
    log_step = -jnp.exp(decay_log) * step_size + decay_extra.T
    glu = value_rows.astype(jnp.float32) * jax.nn.sigmoid(gate_rows.astype(jnp.float32))
    long_mix = causal_conv(glu, long_taps)
    mean = lax.optimization_barrier(jnp.mean(long_mix, axis=1, keepdims=True))
    spread = lax.optimization_barrier(jnp.mean(long_mix * long_mix, axis=1, keepdims=True)) - mean * mean
    conv_out = jax.nn.silu((long_mix - mean) * lax.rsqrt(spread + eps_norm) * conv_gain).astype(jnp.bfloat16)
    input_act = jax.nn.silu(causal_conv(input_rows.astype(jnp.float32), input_taps))
    write_activation = jax.nn.silu(causal_conv(write_rows.astype(jnp.float32), write_taps))
    read_act = jax.nn.silu(causal_conv(read_rows.astype(jnp.float32), fetch_kernel_coefficients))
    per_group = HEADS // GROUPS
    blocks = length // SPAN
    x_heads = (input_act.reshape(length, HEADS, HEAD_P) * step_size[:, :, None]).reshape(blocks, SPAN, HEADS, HEAD_P)
    write_heads = jnp.repeat(write_activation.reshape(length, GROUPS, STATE), per_group, axis=1).reshape(blocks, SPAN, HEADS, STATE)
    read_heads = jnp.repeat(read_act.reshape(length, GROUPS, STATE), per_group, axis=1).reshape(blocks, SPAN, HEADS, STATE)
    log_blocks = log_step.reshape(blocks, SPAN, HEADS)
    ending, outputs = lax.scan(span_step, initial_state, (x_heads, write_heads, read_heads, log_blocks))
    gated = outputs.reshape(length, D_INNER) * jax.nn.silu(gate_z.astype(jnp.float32))
    state_out = (gated * lax.rsqrt(lax.optimization_barrier(jnp.mean(gated * gated, axis=1, keepdims=True)) + eps_norm) * state_gain).astype(jnp.bfloat16)
    pieces = N_FS * N_TP
    conv_width = C_CH // pieces
    state_width = D_INNER // pieces
    contract = (((1,), (1,)), ((), ()))

    def summand_term(total, index):
        conv_part = lax.dynamic_slice_in_dim(conv_out, (index * conv_width).astype(jnp.int32), conv_width, 1)
        conv_back = lax.dynamic_slice_in_dim(conv_output, (index * conv_width).astype(jnp.int32), conv_width, 1)
        state_part = lax.dynamic_slice_in_dim(state_out, (index * state_width).astype(jnp.int32), state_width, 1)
        state_back = lax.dynamic_slice_in_dim(state_output, (index * state_width).astype(jnp.int32), state_width, 1)
        term = lax.dot_general(conv_part, conv_back, contract, preferred_element_type=jnp.float32)
        term = term + lax.dot_general(state_part, state_back, contract, preferred_element_type=jnp.float32)
        rounded = lax.optimization_barrier(term.astype(jnp.bfloat16))
        return (total + rounded.astype(jnp.float32), None)
    total, ignored = lax.scan(summand_term, jnp.zeros((length, D), jnp.float32), jnp.arange(pieces, dtype=jnp.int32))
    return total.astype(jnp.bfloat16)
```

```python
import functools

import jax
import jax.numpy as jnp
from jax import lax
from jax.experimental import pallas as pl
from jax.experimental.pallas import tpu as pltpu
from jax.sharding import PartitionSpec as P

C_CH = 1024
STATE = 128
WIDE_TAPS = 31
SHORT_TAPS = 4
SPAN = 64
D_INNER = 1024


eps_norm = 1e-06


def causal_valid(padded, taps):
    result = lax.conv_general_dilated(
        padded[None],
        taps[:, None, :],
        window_strides=(1,),
        padding="VALID",
        dimension_numbers=("NWC", "WIO", "NWC"),
        feature_group_count=taps.shape[1],
        precision=lax.Precision.HIGHEST,
    )
    return result[0]


MESH = pl.DeviceIdType.MESH
VMEM = pl.BlockSpec(memory_space=pltpu.VMEM)
VMEM_LIMIT = 56 * 1024 * 1024
EDGE = 32
PROJECTED = 6
HALO = 5
COLUMN_CHUNKS = 4


def gather_kernel(n, *refs):
    tokens, gain, steps = refs[:3]
    parts = refs[3:11]
    rows_out, step_out, back_conv, back_state, before = refs[11:16]
    normed, held, edge, send_sem, recv_sem, halo_send, halo_recv = refs[16:]
    me = lax.axis_index("sp")
    chunks = len(parts)
    has_left, has_right = me > 0, me < n - 1
    barrier = pltpu.get_barrier_semaphore()

    @pl.when(has_left)
    def _():
        pl.semaphore_signal(barrier, inc=1, device_id={"sp": me - 1}, device_id_type=MESH)

    @pl.when(has_right)
    def _():
        pl.semaphore_signal(barrier, inc=1, device_id={"sp": me + 1}, device_id_type=MESH)

    pl.semaphore_wait(barrier, jnp.minimum(me, 1) + jnp.minimum(n - 1 - me, 1))

    def link(src, chunk, block, way):
        return pltpu.make_async_remote_copy(
            src_ref=src,
            dst_ref=held.at[chunk, block],
            send_sem=send_sem.at[chunk, way],
            recv_sem=recv_sem.at[chunk, block],
            device_id={"sp": me + 1 if way == 0 else me - 1},
            device_id_type=MESH,
        )

    def send_own(chunk):
        @pl.when(has_right)
        def _():
            link(parts[chunk], chunk, me, 0).start()

        @pl.when(has_left)
        def _():
            link(parts[chunk], chunk, me, 1).start()

    def relay(chunk):
        def hop(d, carry):
            for way, source, more in ((0, me - d, has_right), (1, me + d, has_left)):
                valid = (source >= 0) if way == 0 else (source < n)

                @pl.when(valid)
                def _():
                    copy = link(held.at[chunk, source], chunk, source, way)
                    copy.wait_recv()

                    @pl.when(more)
                    def _():
                        copy.wait_send()
                        copy.start()

            return carry

        lax.fori_loop(1, n, hop, 0, unroll=n <= 8)

    ahead = 2
    for chunk in range(ahead):
        send_own(chunk)
    values = tokens[...].astype(jnp.float32)
    scale = lax.rsqrt(jnp.mean(values * values, axis=1, keepdims=True) + eps_norm)
    normed[...] = (values * scale * gain[...]).astype(jnp.bfloat16)
    step_out[...] = jnp.dot(normed[...], steps[...], preferred_element_type=jnp.float32)
    for chunk in range(chunks):
        held[chunk, me] = parts[chunk][...]
    rows = tokens.shape[0]
    width = parts[0].shape[1]
    depth = parts[0].shape[0]
    for chunk in range(chunks):
        if chunk + ahead < chunks:
            send_own(chunk + ahead)
        relay(chunk)
        if chunk < PROJECTED:
            whole = held[chunk].reshape(n * depth, width)
            rows_out[chunk] = jnp.dot(
                normed[...], whole, preferred_element_type=jnp.float32
            ).astype(jnp.bfloat16)
        if chunk == HALO - 1:
            edge[...] = rows_out[:HALO, rows - EDGE :, :]
        if chunk == HALO:

            @pl.when(has_right)
            def _():
                halo(edge, before, halo_send, halo_recv, me + 1).start()

    back_conv[...] = held[PROJECTED].reshape(n * depth, width)
    back_state[...] = held[PROJECTED + 1].reshape(n * depth, width)

    @pl.when(has_left)
    def _():
        halo(edge, before, halo_send, halo_recv, me + 1).wait_recv()

    @pl.when(me == 0)
    def _():
        before[...] = jnp.zeros_like(before)

    @pl.when(has_right)
    def _():
        halo(edge, before, halo_send, halo_recv, me + 1).wait_send()

    for chunk in range(chunks):

        @pl.when(has_right)
        def _():
            link(parts[chunk], chunk, me, 0).wait_send()

        @pl.when(has_left)
        def _():
            link(parts[chunk], chunk, me, 1).wait_send()


def halo(edge, before, send, recv, target):
    return pltpu.make_async_remote_copy(
        src_ref=edge,
        dst_ref=before,
        send_sem=send,
        recv_sem=recv,
        device_id={"sp": target},
        device_id_type=MESH,
    )


def gathered_rows(tokens, gain, steps, weights):
    n = lax.axis_size("sp")
    rows = tokens.shape[0]
    depth, width = weights[0].shape
    chunks = len(weights)
    bf16 = jnp.bfloat16
    return pl.pallas_call(
        functools.partial(gather_kernel, n),
        out_shape=(
            jax.ShapeDtypeStruct((PROJECTED, rows, width), bf16),
            jax.ShapeDtypeStruct((rows, steps.shape[1]), jnp.float32),
            jax.ShapeDtypeStruct((n * depth, width), bf16),
            jax.ShapeDtypeStruct((n * depth, width), bf16),
            jax.ShapeDtypeStruct((HALO, EDGE, width), bf16),
        ),
        in_specs=[VMEM] * (3 + chunks),
        out_specs=(VMEM,) * 5,
        scratch_shapes=[
            pltpu.VMEM(tokens.shape, bf16),
            pltpu.VMEM((chunks, n, depth, width), bf16),
            pltpu.VMEM((HALO, EDGE, width), bf16),
            pltpu.SemaphoreType.DMA((chunks, 2)),
            pltpu.SemaphoreType.DMA((chunks, n)),
            pltpu.SemaphoreType.DMA,
            pltpu.SemaphoreType.DMA,
        ],
        compiler_params=pltpu.CompilerParams(
            collective_id=0, has_side_effects=True, vmem_limit_bytes=VMEM_LIMIT
        ),
    )(tokens, gain[None, :], steps, *weights)


def peer_id(axes, sizes, index):
    if len(axes) == 1:
        return {axes[0]: index}
    return {axes[0]: index // sizes[1], axes[1]: index % sizes[1]}


def greet(axes, sizes, me, n):
    barrier = pltpu.get_barrier_semaphore()
    for i in range(1, n):
        pl.semaphore_signal(
            barrier,
            inc=1,
            device_id=peer_id(axes, sizes, lax.rem(me + i, n)),
            device_id_type=MESH,
        )
    pl.semaphore_wait(barrier, n - 1)


def index_of(axes, sizes):
    me = lax.axis_index(axes[0])
    return me if len(axes) == 1 else me * sizes[1] + lax.axis_index(axes[1])


def exchange_kernel(axes, sizes, count, add, *refs):
    ins, outs, lands = refs[:count], refs[count : 2 * count], refs[2 * count : 3 * count]
    send_sem, recv_sem = refs[3 * count :]
    n = 1
    for size in sizes:
        n *= size
    me = index_of(axes, sizes)
    greet(axes, sizes, me, n)

    def copy(k, slot, target):
        return pltpu.make_async_remote_copy(
            src_ref=ins[k],
            dst_ref=lands[k].at[slot],
            send_sem=send_sem.at[k, slot],
            recv_sem=recv_sem.at[k, slot],
            device_id=peer_id(axes, sizes, target),
            device_id_type=MESH,
        )

    for i in range(1, n):
        for k in range(count):
            pltpu.make_async_remote_copy(
                src_ref=ins[k],
                dst_ref=lands[k].at[me],
                send_sem=send_sem.at[k, lax.rem(me + i, n)],
                recv_sem=recv_sem.at[k, me],
                device_id=peer_id(axes, sizes, lax.rem(me + i, n)),
                device_id_type=MESH,
            ).start()
    for k in range(count):
        lands[k][me] = ins[k][...]
    for i in range(1, n):
        for k in range(count):
            copy(k, lax.rem(me + n - i, n), lax.rem(me + n - i, n)).wait_recv()
    for k in range(count):
        if add:
            total = lands[k][0]
            for i in range(1, n):
                total = total + lands[k][i]
            outs[k][...] = total
        else:
            outs[k][...] = lands[k][...]
    for i in range(1, n):
        for k in range(count):
            copy(k, lax.rem(me + i, n), lax.rem(me + i, n)).wait_send()


def exchanged(arrays, axes, add, number):
    sizes = tuple(lax.axis_size(a) for a in axes)
    n = 1
    for size in sizes:
        n *= size
    count = len(arrays)
    out = [
        jax.ShapeDtypeStruct(a.shape if add else (n,) + a.shape, a.dtype) for a in arrays
    ]
    return pl.pallas_call(
        functools.partial(exchange_kernel, axes, sizes, count, add),
        out_shape=tuple(out),
        in_specs=[VMEM] * count,
        out_specs=(VMEM,) * count,
        scratch_shapes=[pltpu.VMEM((n,) + a.shape, a.dtype) for a in arrays]
        + [pltpu.SemaphoreType.DMA((count, n)), pltpu.SemaphoreType.DMA((count, n))],
        compiler_params=pltpu.CompilerParams(
            collective_id=number, has_side_effects=True, vmem_limit_bytes=VMEM_LIMIT
        ),
    )(*arrays)


def project_kernel(sizes, conv, state, back_conv, back_state, out, *scratch):
    core_out, core_in, plane_out, plane_in, own = scratch[:5]
    core_send, core_recv, plane_send, plane_recv = scratch[5:]
    n_fs, n_tp = sizes
    fs, tp = lax.axis_index("fs"), lax.axis_index("tp")
    me = fs * n_tp + tp
    greet(("fs", "tp"), sizes, me, n_fs * n_tp)
    block = conv.shape[2]
    wide = back_conv.shape[0] // COLUMN_CHUNKS
    contract = (((1,), (1,)), ((), ()))

    def term(core, j):
        left = jnp.concatenate([conv[f, core] for f in range(n_fs)], axis=0)
        right = jnp.concatenate([state[f, core] for f in range(n_fs)], axis=0)
        at = pl.ds(j * wide, wide)
        return lax.dot_general(
            left, back_conv[at, :], contract, preferred_element_type=jnp.float32
        ) + lax.dot_general(
            right, back_state[at, :], contract, preferred_element_type=jnp.float32
        )

    def core_copy(step, j):
        target = lax.rem(tp + step, n_tp)
        return pltpu.make_async_remote_copy(
            src_ref=core_out.at[step - 1, j],
            dst_ref=core_in.at[step - 1, j],
            send_sem=core_send.at[step - 1, j],
            recv_sem=core_recv.at[step - 1, j],
            device_id={"tp": target},
            device_id_type=MESH,
        )

    def plane_copy(step, j):
        target = lax.rem(fs + step, n_fs)
        return pltpu.make_async_remote_copy(
            src_ref=plane_out.at[target, j],
            dst_ref=plane_in.at[step - 1, j],
            send_sem=plane_send.at[step - 1, j],
            recv_sem=plane_recv.at[step - 1, j],
            device_id={"fs": target},
            device_id_type=MESH,
        )

    def send_core(j):
        for step in range(1, n_tp):
            core_copy(step, j).start()

    def send_plane(j):
        for step in range(1, n_fs):
            plane_copy(step, j).start()

    for j in range(COLUMN_CHUNKS):
        for step in range(1, n_tp):
            core_out[step - 1, j] = term(lax.rem(tp + step, n_tp), j).astype(jnp.bfloat16)
        if j:
            send_core(j - 1)
    mine = term(tp, 0)
    send_core(COLUMN_CHUNKS - 1)
    for j in range(COLUMN_CHUNKS):
        total = mine
        for step in range(1, n_tp):
            core_copy(step, j).wait_recv()
            total = total + core_in[step - 1, j].astype(jnp.float32)
        for f in range(n_fs):
            part = total[f * block : (f + 1) * block]
            plane_out[f, j] = part.astype(jnp.bfloat16)

            @pl.when(f == fs)
            def _():
                own[j] = part

        if j + 1 < COLUMN_CHUNKS:
            mine = term(tp, j + 1)
        send_plane(j)
    for j in range(COLUMN_CHUNKS):
        total = own[j]
        for step in range(1, n_fs):
            plane_copy(step, j).wait_recv()
            total = total + plane_in[step - 1, j].astype(jnp.float32)
        out[:, j * wide : (j + 1) * wide] = total.astype(jnp.bfloat16)
    for j in range(COLUMN_CHUNKS):
        for step in range(1, n_tp):
            core_copy(step, j).wait_send()
        for step in range(1, n_fs):
            plane_copy(step, j).wait_send()


def projected(conv, state, back_conv, back_state):
    n_fs, n_tp = sizes = (lax.axis_size("fs"), lax.axis_size("tp"))
    rows, width = conv.shape
    block = rows // (n_fs * n_tp)
    features = back_conv.shape[0]
    wide = features // COLUMN_CHUNKS
    k = COLUMN_CHUNKS
    bf16 = jnp.bfloat16
    shaped = (n_fs, n_tp, block, width)
    return pl.pallas_call(
        functools.partial(project_kernel, sizes),
        out_shape=jax.ShapeDtypeStruct((block, features), bf16),
        in_specs=[VMEM] * 4,
        out_specs=VMEM,
        scratch_shapes=[
            pltpu.VMEM((n_tp - 1, k, n_fs * block, wide), bf16),
            pltpu.VMEM((n_tp - 1, k, n_fs * block, wide), bf16),
            pltpu.VMEM((n_fs, k, block, wide), bf16),
            pltpu.VMEM((n_fs - 1, k, block, wide), bf16),
            pltpu.VMEM((k, block, wide), jnp.float32),
            pltpu.SemaphoreType.DMA((n_tp - 1, k)),
            pltpu.SemaphoreType.DMA((n_tp - 1, k)),
            pltpu.SemaphoreType.DMA((n_fs - 1, k)),
            pltpu.SemaphoreType.DMA((n_fs - 1, k)),
        ],
        compiler_params=pltpu.CompilerParams(
            collective_id=4, has_side_effects=True, vmem_limit_bytes=VMEM_LIMIT
        ),
    )(conv.reshape(shaped), state.reshape(shaped), back_conv, back_state)


def carry_step(state, inputs):
    fresh, last = inputs
    return (state * jnp.exp(last)[:, None, None] + fresh, state)


def per_device(
    tokens,
    norm_gain,
    conv_value,
    conv_gate,
    mixer_gate,
    state_input,
    write_projection,
    state_read,
    step_proj,
    step_bias,
    decay_log,
    decay_extra,
    input_taps,
    write_taps,
    fetch_kernel_coefficients,
    long_taps,
    conv_gain,
    state_gain,
    conv_output,
    state_output,
    initial_state,
):
    rows = tokens.shape[0]
    channels = conv_value.shape[1]
    width_in = state_input.shape[1]
    width_group = write_projection.shape[1]
    heads = step_bias.shape[0]
    groups = width_group // STATE
    per_group = heads // groups
    head_size = width_in // heads
    projected_rows, step_all, back_conv, back_state, before = gathered_rows(
        tokens,
        norm_gain,
        step_proj,
        (
            state_input,
            write_projection,
            state_read,
            conv_value,
            conv_gate,
            mixer_gate,
            conv_output,
            state_output,
        ),
    )
    input_rows, write_rows, read_rows, value_rows, gate_rows, gate_z = (
        projected_rows[i] for i in range(PROJECTED)
    )
    head_start = (lax.axis_index("fs") * lax.axis_size("tp") + lax.axis_index("tp")) * heads
    step_raw = lax.dynamic_slice_in_dim(step_all, head_start, heads, 1)
    step_size = jax.nn.softplus(step_raw + step_bias)
    log_step = -jnp.exp(decay_log) * step_size + decay_extra.T
    drop = EDGE - WIDE_TAPS + 1
    short_edge = jnp.concatenate(
        [before[i, EDGE - SHORT_TAPS + 1 :] for i in range(3)], axis=1
    )
    state_row_values = jnp.concatenate([input_rows, write_rows, read_rows], axis=1)
    state_full = jnp.concatenate([short_edge, state_row_values], axis=0).astype(jnp.float32)
    state_taps = jnp.concatenate([input_taps, write_taps, fetch_kernel_coefficients], axis=1)
    activated = jax.nn.silu(causal_valid(state_full, state_taps))
    input_act = activated[:, :width_in]
    write_activation = activated[:, width_in : width_in + width_group]
    read_act = activated[:, width_in + width_group :]
    blocks = rows // SPAN
    x_heads = (input_act.reshape(rows, heads, head_size) * step_size[:, :, None]).reshape(
        blocks, SPAN, heads, head_size
    )
    write_heads = jnp.repeat(
        write_activation.reshape(rows, groups, STATE), per_group, axis=1
    ).reshape(blocks, SPAN, heads, STATE)
    read_heads = jnp.repeat(read_act.reshape(rows, groups, STATE), per_group, axis=1).reshape(
        blocks, SPAN, heads, STATE
    )
    log_blocks = log_step.reshape(blocks, SPAN, heads)
    cumul = jnp.cumsum(log_blocks, axis=1)
    lower = jnp.tril(jnp.ones((SPAN, SPAN), dtype=bool))
    by_head = jnp.swapaxes(cumul, 1, 2)
    gaps = by_head[:, :, :, None] - by_head[:, :, None, :]
    weights = jnp.where(lower, jnp.exp(jnp.where(lower, gaps, 0.0)), 0.0)
    scores = jnp.einsum("bthn,bshn->bhts", read_heads, write_heads, precision=lax.Precision.HIGHEST)
    inner = jnp.einsum(
        "bhts,bshp->bthp", scores * weights, x_heads, precision=lax.Precision.HIGHEST
    )
    last = cumul[:, -1]
    fresh = jnp.einsum(
        "bshn,bshp->bhpn",
        write_heads * jnp.exp(last[:, None, :] - cumul)[:, :, :, None],
        x_heads,
        precision=lax.Precision.HIGHEST,
    )
    state_end, block_states = lax.scan(
        carry_step, jnp.zeros((heads, head_size, STATE), jnp.float32), (fresh, last)
    )
    logsum = jnp.sum(last, axis=0)
    block_prefix = jnp.cumsum(last, axis=0) - last
    start_decay = jnp.exp(block_prefix[:, None, :] + cumul)
    local_out = (
        inner
        + jnp.einsum("bthn,bhpn->bthp", read_heads, block_states, precision=lax.Precision.HIGHEST)
        * jnp.exp(cumul)[:, :, :, None]
    )
    value_full = jnp.concatenate([before[3, drop:], value_rows], axis=0).astype(jnp.float32)
    gate_full = jnp.concatenate([before[4, drop:], gate_rows], axis=0).astype(
        jnp.float32
    )
    glu = value_full * jax.nn.sigmoid(gate_full)
    long_mix = causal_valid(glu, long_taps)
    moments = jnp.stack([jnp.sum(long_mix, axis=1), jnp.sum(long_mix * long_mix, axis=1)])
    (moments,) = exchanged((moments,), ("fs", "tp"), True, 1)
    total_sum, total_square = moments[0], moments[1]
    mean = total_sum / C_CH
    spread = total_square / C_CH - mean * mean
    conv_out = jax.nn.silu(
        (long_mix - mean[:, None]) * lax.rsqrt(spread + eps_norm)[:, None] * conv_gain
    ).astype(jnp.bfloat16)
    piece, totals = exchanged(
        (
            state_end.astype(jnp.bfloat16),
            jnp.broadcast_to(logsum[:, None], (heads, STATE)),
        ),
        ("sp",),
        False,
        3,
    )
    piece = piece.astype(jnp.float32)
    totals = totals[:, :, 0]
    inclusive = jnp.cumsum(totals, axis=0)
    position = lax.axis_index("sp")
    prefix_log = lax.dynamic_index_in_dim(inclusive - totals, position, 0, keepdims=False)
    count = piece.shape[0]
    order = jnp.arange(count, dtype=jnp.int32)
    live = (order < position)[:, None]
    factor = jnp.where(live, jnp.exp(jnp.where(live, prefix_log[None, :] - inclusive, 0.0)), 0.0)
    entering = jnp.zeros_like(state_end) + jnp.einsum(
        "kh,khpn->hpn", factor, piece, precision=lax.Precision.HIGHEST
    )
    start_state = entering + jnp.exp(prefix_log)[:, None, None] * initial_state
    outputs = (
        local_out
        + jnp.einsum("bthn,hpn->bthp", read_heads, start_state, precision=lax.Precision.HIGHEST)
        * start_decay[:, :, :, None]
    )
    gated = outputs.reshape(rows, width_in) * jax.nn.silu(gate_z.astype(jnp.float32))
    (quadratic_total,) = exchanged(
        (jnp.sum(gated * gated, axis=1)[None, :],), ("fs", "tp"), True, 2
    )
    quadratic_total = quadratic_total[0]
    state_out = (
        gated * lax.rsqrt(quadratic_total / D_INNER + eps_norm)[:, None] * state_gain
    ).astype(jnp.bfloat16)
    return projected(conv_out, state_out, back_conv, back_state)


def solution(mesh):
    placed = (
        P("sp", None),
        P(),
        P("sp", ("fs", "tp")),
        P("sp", ("fs", "tp")),
        P("sp", ("fs", "tp")),
        P("sp", ("fs", "tp")),
        P("sp", ("fs", "tp")),
        P("sp", ("fs", "tp")),
        P(),
        P(("fs", "tp")),
        P(("fs", "tp")),
        P(("fs", "tp"), "sp"),
        P(None, ("fs", "tp")),
        P(None, ("fs", "tp")),
        P(None, ("fs", "tp")),
        P(None, ("fs", "tp")),
        P(("fs", "tp")),
        P(("fs", "tp")),
        P("sp", ("fs", "tp")),
        P("sp", ("fs", "tp")),
        P(("fs", "tp"), None, None),
    )
    return jax.shard_map(
        per_device,
        mesh=mesh,
        in_specs=placed,
        out_specs=P(("sp", "fs", "tp"), None),
        check_vma=False,
    )
```

```python
import functools

import jax
import jax.numpy as jnp
from jax import lax
from jax.experimental import pallas as pl
from jax.experimental.pallas import tpu as pltpu
from jax.sharding import PartitionSpec as P

C_CH = 1024
STATE = 128
WIDE_TAPS = 31
SHORT_TAPS = 4
SPAN = 64
D_INNER = 1024


eps_norm = 1e-06


def causal_valid(padded, taps):
    result = lax.conv_general_dilated(
        padded[None],
        taps[:, None, :],
        window_strides=(1,),
        padding="VALID",
        dimension_numbers=("NWC", "WIO", "NWC"),
        feature_group_count=taps.shape[1],
        precision=lax.Precision.HIGHEST,
    )
    return result[0]


MESH = pl.DeviceIdType.MESH
VMEM = pl.BlockSpec(memory_space=pltpu.VMEM)
VMEM_LIMIT = 56 * 1024 * 1024
EDGE = 32
PROJECTED = 6
HALO = 5
COLUMN_CHUNKS = 4


def gather_kernel(n, *refs):
    tokens, gain, steps = refs[:3]
    parts = refs[3:11]
    rows_out, step_out, back_conv, back_state, before = refs[11:16]
    normed, held, edge, send_sem, recv_sem, halo_send, halo_recv = refs[16:]
    me = lax.axis_index("sp")
    chunks = len(parts)
    has_left, has_right = me > 0, me < n - 1
    barrier = pltpu.get_barrier_semaphore()

    @pl.when(has_left)
    def _():
        pl.semaphore_signal(barrier, inc=1, device_id={"sp": me - 1}, device_id_type=MESH)

    @pl.when(has_right)
    def _():
        pl.semaphore_signal(barrier, inc=1, device_id={"sp": me + 1}, device_id_type=MESH)

    pl.semaphore_wait(barrier, jnp.minimum(me, 1) + jnp.minimum(n - 1 - me, 1))

    def link(src, chunk, block, way):
        return pltpu.make_async_remote_copy(
            src_ref=src,
            dst_ref=held.at[chunk, block],
            send_sem=send_sem.at[chunk, way],
            recv_sem=recv_sem.at[chunk, block],
            device_id={"sp": me + 1 if way == 0 else me - 1},
            device_id_type=MESH,
        )

    def send_own(chunk):
        @pl.when(has_right)
        def _():
            link(parts[chunk], chunk, me, 0).start()

        @pl.when(has_left)
        def _():
            link(parts[chunk], chunk, me, 1).start()

    def relay(chunk):
        def hop(d, carry):
            for way, source, more in ((0, me - d, has_right), (1, me + d, has_left)):
                valid = (source >= 0) if way == 0 else (source < n)

                @pl.when(valid)
                def _():
                    copy = link(held.at[chunk, source], chunk, source, way)
                    copy.wait_recv()

                    @pl.when(more)
                    def _():
                        copy.wait_send()
                        copy.start()

            return carry

        lax.fori_loop(1, n, hop, 0, unroll=n <= 8)

    ahead = chunks
    for chunk in range(ahead):
        send_own(chunk)
    values = tokens[...].astype(jnp.float32)
    scale = lax.rsqrt(jnp.mean(values * values, axis=1, keepdims=True) + eps_norm)
    normed[...] = (values * scale * gain[...]).astype(jnp.bfloat16)
    step_out[...] = jnp.dot(normed[...], steps[...], preferred_element_type=jnp.float32)
    for chunk in range(chunks):
        held[chunk, me] = parts[chunk][...]
    rows = tokens.shape[0]
    width = parts[0].shape[1]
    depth = parts[0].shape[0]
    for chunk in range(chunks):
        if chunk + ahead < chunks:
            send_own(chunk + ahead)
        relay(chunk)
        if chunk < PROJECTED:
            whole = held[chunk].reshape(n * depth, width)
            rows_out[chunk] = jnp.dot(
                normed[...], whole, preferred_element_type=jnp.float32
            ).astype(jnp.bfloat16)
        if chunk == HALO - 1:
            edge[...] = rows_out[:HALO, rows - EDGE :, :]
        if chunk == HALO:

            @pl.when(has_right)
            def _():
                halo(edge, before, halo_send, halo_recv, me + 1).start()

    back_conv[...] = held[PROJECTED].reshape(n * depth, width)
    back_state[...] = held[PROJECTED + 1].reshape(n * depth, width)

    @pl.when(has_left)
    def _():
        halo(edge, before, halo_send, halo_recv, me + 1).wait_recv()

    @pl.when(me == 0)
    def _():
        before[...] = jnp.zeros_like(before)

    @pl.when(has_right)
    def _():
        halo(edge, before, halo_send, halo_recv, me + 1).wait_send()

    for chunk in range(chunks):

        @pl.when(has_right)
        def _():
            link(parts[chunk], chunk, me, 0).wait_send()

        @pl.when(has_left)
        def _():
            link(parts[chunk], chunk, me, 1).wait_send()


def halo(edge, before, send, recv, target):
    return pltpu.make_async_remote_copy(
        src_ref=edge,
        dst_ref=before,
        send_sem=send,
        recv_sem=recv,
        device_id={"sp": target},
        device_id_type=MESH,
    )


def gathered_rows(tokens, gain, steps, weights):
    n = lax.axis_size("sp")
    rows = tokens.shape[0]
    depth, width = weights[0].shape
    chunks = len(weights)
    bf16 = jnp.bfloat16
    return pl.pallas_call(
        functools.partial(gather_kernel, n),
        out_shape=(
            jax.ShapeDtypeStruct((PROJECTED, rows, width), bf16),
            jax.ShapeDtypeStruct((rows, steps.shape[1]), jnp.float32),
            jax.ShapeDtypeStruct((n * depth, width), bf16),
            jax.ShapeDtypeStruct((n * depth, width), bf16),
            jax.ShapeDtypeStruct((HALO, EDGE, width), bf16),
        ),
        in_specs=[VMEM] * (3 + chunks),
        out_specs=(VMEM,) * 5,
        scratch_shapes=[
            pltpu.VMEM(tokens.shape, bf16),
            pltpu.VMEM((chunks, n, depth, width), bf16),
            pltpu.VMEM((HALO, EDGE, width), bf16),
            pltpu.SemaphoreType.DMA((chunks, 2)),
            pltpu.SemaphoreType.DMA((chunks, n)),
            pltpu.SemaphoreType.DMA,
            pltpu.SemaphoreType.DMA,
        ],
        compiler_params=pltpu.CompilerParams(
            collective_id=0, has_side_effects=True, vmem_limit_bytes=VMEM_LIMIT
        ),
    )(tokens, gain[None, :], steps, *weights)


def peer_id(axes, sizes, index):
    if len(axes) == 1:
        return {axes[0]: index}
    return {axes[0]: index // sizes[1], axes[1]: index % sizes[1]}


def greet(axes, sizes, me, n):
    barrier = pltpu.get_barrier_semaphore()
    for i in range(1, n):
        pl.semaphore_signal(
            barrier,
            inc=1,
            device_id=peer_id(axes, sizes, lax.rem(me + i, n)),
            device_id_type=MESH,
        )
    pl.semaphore_wait(barrier, n - 1)


def index_of(axes, sizes):
    me = lax.axis_index(axes[0])
    return me if len(axes) == 1 else me * sizes[1] + lax.axis_index(axes[1])


def exchange_kernel(groups, *refs):
    count = len(groups)
    ins, outs, lands = refs[:count], refs[count : 2 * count], refs[2 * count : 3 * count]
    sems = refs[3 * count :]
    barrier = pltpu.get_barrier_semaphore()
    greeted = set()
    expected = 0
    for axes, sizes, n, add in groups:
        if axes in greeted:
            continue
        greeted.add(axes)
        me = index_of(axes, sizes)
        for i in range(1, n):
            pl.semaphore_signal(
                barrier,
                inc=1,
                device_id=peer_id(axes, sizes, lax.rem(me + i, n)),
                device_id_type=MESH,
            )
        expected += n - 1
    pl.semaphore_wait(barrier, expected)

    def copy(k, slot, land, target):
        axes, sizes, n, add = groups[k]
        return pltpu.make_async_remote_copy(
            src_ref=ins[k],
            dst_ref=lands[k].at[land],
            send_sem=sems[2 * k].at[slot],
            recv_sem=sems[2 * k + 1].at[land],
            device_id=peer_id(axes, sizes, target),
            device_id_type=MESH,
        )

    for k, (axes, sizes, n, add) in enumerate(groups):
        me = index_of(axes, sizes)
        for i in range(1, n):
            target = lax.rem(me + i, n)
            copy(k, target, me, target).start()
    for k, (axes, sizes, n, add) in enumerate(groups):
        me = index_of(axes, sizes)
        lands[k][me] = ins[k][...]
        for i in range(1, n):
            source = lax.rem(me + n - i, n)
            copy(k, source, source, source).wait_recv()
        if add:
            total = lands[k][0]
            for i in range(1, n):
                total = total + lands[k][i]
            outs[k][...] = total
        else:
            outs[k][...] = lands[k][...]
    for k, (axes, sizes, n, add) in enumerate(groups):
        me = index_of(axes, sizes)
        for i in range(1, n):
            target = lax.rem(me + i, n)
            copy(k, target, me, target).wait_send()


def exchanged(arrays, plans, number):
    groups, out, lands, sems = [], [], [], []
    for array, (axes, add) in zip(arrays, plans):
        sizes = tuple(lax.axis_size(a) for a in axes)
        n = 1
        for size in sizes:
            n *= size
        groups.append((axes, sizes, n, add))
        shape = (n,) + array.shape
        out.append(jax.ShapeDtypeStruct(array.shape if add else shape, array.dtype))
        lands.append(pltpu.VMEM(shape, array.dtype))
        sems += [pltpu.SemaphoreType.DMA((n,)), pltpu.SemaphoreType.DMA((n,))]
    count = len(arrays)
    return pl.pallas_call(
        functools.partial(exchange_kernel, tuple(groups)),
        out_shape=tuple(out),
        in_specs=[VMEM] * count,
        out_specs=(VMEM,) * count,
        scratch_shapes=lands + sems,
        compiler_params=pltpu.CompilerParams(
            collective_id=number, has_side_effects=True, vmem_limit_bytes=VMEM_LIMIT
        ),
    )(*arrays)


def project_kernel(sizes, conv, gated, square, gain, back_conv, back_state, out, *scratch):
    core_out, core_in, plane_out, plane_in, own = scratch[:5]
    core_send, core_recv, plane_send, plane_recv = scratch[5:9]
    state, squares, square_send, square_recv = scratch[9:]
    n_fs, n_tp = sizes
    fs, tp = lax.axis_index("fs"), lax.axis_index("tp")
    me = fs * n_tp + tp
    n = n_fs * n_tp
    greet(("fs", "tp"), sizes, me, n)

    def square_copy(slot, land, target):
        return pltpu.make_async_remote_copy(
            src_ref=square,
            dst_ref=squares.at[land],
            send_sem=square_send.at[slot],
            recv_sem=square_recv.at[land],
            device_id=peer_id(("fs", "tp"), sizes, target),
            device_id_type=MESH,
        )

    for i in range(1, n):
        target = lax.rem(me + i, n)
        square_copy(target, me, target).start()
    squares[me] = square[...]
    for i in range(1, n):
        source = lax.rem(me + n - i, n)
        square_copy(source, source, source).wait_recv()
    whole = squares[0]
    for i in range(1, n):
        whole = whole + squares[i]
    factor = lax.rsqrt(whole / D_INNER + eps_norm)
    factor = jnp.broadcast_to(factor, (8, factor.shape[1])).T[:, :1]
    rows = conv.shape[2]
    for f in range(n_fs):
        for c in range(n_tp):
            at = (f * n_tp + c) * rows
            state[f, c] = (gated[f, c] * factor[at : at + rows] * gain[...]).astype(jnp.bfloat16)
    block = conv.shape[2]
    wide = back_conv.shape[0] // COLUMN_CHUNKS
    contract = (((1,), (1,)), ((), ()))

    def term(core, j):
        left = jnp.concatenate([conv[f, core] for f in range(n_fs)], axis=0)
        right = jnp.concatenate([state[f, core] for f in range(n_fs)], axis=0)
        at = pl.ds(j * wide, wide)
        return lax.dot_general(
            left, back_conv[at, :], contract, preferred_element_type=jnp.float32
        ) + lax.dot_general(
            right, back_state[at, :], contract, preferred_element_type=jnp.float32
        )

    def core_copy(step, j):
        target = lax.rem(tp + step, n_tp)
        return pltpu.make_async_remote_copy(
            src_ref=core_out.at[step - 1, j],
            dst_ref=core_in.at[step - 1, j],
            send_sem=core_send.at[step - 1, j],
            recv_sem=core_recv.at[step - 1, j],
            device_id={"tp": target},
            device_id_type=MESH,
        )

    def plane_copy(step, j):
        target = lax.rem(fs + step, n_fs)
        return pltpu.make_async_remote_copy(
            src_ref=plane_out.at[target, j],
            dst_ref=plane_in.at[step - 1, j],
            send_sem=plane_send.at[step - 1, j],
            recv_sem=plane_recv.at[step - 1, j],
            device_id={"fs": target},
            device_id_type=MESH,
        )

    def send_core(j):
        for step in range(1, n_tp):
            core_copy(step, j).start()

    def send_plane(j):
        for step in range(1, n_fs):
            plane_copy(step, j).start()

    for j in range(COLUMN_CHUNKS):
        for step in range(1, n_tp):
            core_out[step - 1, j] = term(lax.rem(tp + step, n_tp), j).astype(jnp.bfloat16)
        if j:
            send_core(j - 1)
    mine = term(tp, 0)
    send_core(COLUMN_CHUNKS - 1)
    for j in range(COLUMN_CHUNKS):
        total = mine
        for step in range(1, n_tp):
            core_copy(step, j).wait_recv()
            total = total + core_in[step - 1, j].astype(jnp.float32)
        for f in range(n_fs):
            part = total[f * block : (f + 1) * block]
            plane_out[f, j] = part.astype(jnp.bfloat16)

            @pl.when(f == fs)
            def _():
                own[j] = part

        if j + 1 < COLUMN_CHUNKS:
            mine = term(tp, j + 1)
        send_plane(j)
    for j in range(COLUMN_CHUNKS):
        total = own[j]
        for step in range(1, n_fs):
            plane_copy(step, j).wait_recv()
            total = total + plane_in[step - 1, j].astype(jnp.float32)
        out[:, j * wide : (j + 1) * wide] = total.astype(jnp.bfloat16)
    for i in range(1, n):
        target = lax.rem(me + i, n)
        square_copy(target, me, target).wait_send()
    for j in range(COLUMN_CHUNKS):
        for step in range(1, n_tp):
            core_copy(step, j).wait_send()
        for step in range(1, n_fs):
            plane_copy(step, j).wait_send()


def projected(conv, gated, square, gain, back_conv, back_state):
    n_fs, n_tp = sizes = (lax.axis_size("fs"), lax.axis_size("tp"))
    rows, width = conv.shape
    block = rows // (n_fs * n_tp)
    features = back_conv.shape[0]
    wide = features // COLUMN_CHUNKS
    k = COLUMN_CHUNKS
    bf16 = jnp.bfloat16
    shaped = (n_fs, n_tp, block, width)
    return pl.pallas_call(
        functools.partial(project_kernel, sizes),
        out_shape=jax.ShapeDtypeStruct((block, features), bf16),
        in_specs=[VMEM] * 6,
        out_specs=VMEM,
        scratch_shapes=[
            pltpu.VMEM((n_tp - 1, k, n_fs * block, wide), bf16),
            pltpu.VMEM((n_tp - 1, k, n_fs * block, wide), bf16),
            pltpu.VMEM((n_fs, k, block, wide), bf16),
            pltpu.VMEM((n_fs - 1, k, block, wide), bf16),
            pltpu.VMEM((k, block, wide), jnp.float32),
            pltpu.SemaphoreType.DMA((n_tp - 1, k)),
            pltpu.SemaphoreType.DMA((n_tp - 1, k)),
            pltpu.SemaphoreType.DMA((n_fs - 1, k)),
            pltpu.SemaphoreType.DMA((n_fs - 1, k)),
            pltpu.VMEM(shaped, bf16),
            pltpu.VMEM((n_fs * n_tp, 1, rows), jnp.float32),
            pltpu.SemaphoreType.DMA((n_fs * n_tp,)),
            pltpu.SemaphoreType.DMA((n_fs * n_tp,)),
        ],
        compiler_params=pltpu.CompilerParams(
            collective_id=4, has_side_effects=True, vmem_limit_bytes=VMEM_LIMIT
        ),
    )(
        conv.reshape(shaped),
        gated.reshape(shaped),
        square[None, :],
        gain[None, :],
        back_conv,
        back_state,
    )


def carry_step(state, inputs):
    fresh, last = inputs
    return (state * jnp.exp(last)[:, None, None] + fresh, state)


def per_device(
    tokens,
    norm_gain,
    conv_value,
    conv_gate,
    mixer_gate,
    state_input,
    write_projection,
    state_read,
    step_proj,
    step_bias,
    decay_log,
    decay_extra,
    input_taps,
    write_taps,
    fetch_kernel_coefficients,
    long_taps,
    conv_gain,
    state_gain,
    conv_output,
    state_output,
    initial_state,
):
    rows = tokens.shape[0]
    channels = conv_value.shape[1]
    width_in = state_input.shape[1]
    width_group = write_projection.shape[1]
    heads = step_bias.shape[0]
    groups = width_group // STATE
    per_group = heads // groups
    head_size = width_in // heads
    projected_rows, step_all, back_conv, back_state, before = gathered_rows(
        tokens,
        norm_gain,
        step_proj,
        (
            state_input,
            write_projection,
            state_read,
            conv_value,
            conv_gate,
            mixer_gate,
            conv_output,
            state_output,
        ),
    )
    input_rows, write_rows, read_rows, value_rows, gate_rows, gate_z = (
        projected_rows[i] for i in range(PROJECTED)
    )
    head_start = (lax.axis_index("fs") * lax.axis_size("tp") + lax.axis_index("tp")) * heads
    step_raw = lax.dynamic_slice_in_dim(step_all, head_start, heads, 1)
    step_size = jax.nn.softplus(step_raw + step_bias)
    log_step = -jnp.exp(decay_log) * step_size + decay_extra.T
    drop = EDGE - WIDE_TAPS + 1
    short_edge = jnp.concatenate(
        [before[i, EDGE - SHORT_TAPS + 1 :] for i in range(3)], axis=1
    )
    state_row_values = jnp.concatenate([input_rows, write_rows, read_rows], axis=1)
    state_full = jnp.concatenate([short_edge, state_row_values], axis=0).astype(jnp.float32)
    state_taps = jnp.concatenate([input_taps, write_taps, fetch_kernel_coefficients], axis=1)
    activated = jax.nn.silu(causal_valid(state_full, state_taps))
    input_act = activated[:, :width_in]
    write_activation = activated[:, width_in : width_in + width_group]
    read_act = activated[:, width_in + width_group :]
    blocks = rows // SPAN
    x_heads = (input_act.reshape(rows, heads, head_size) * step_size[:, :, None]).reshape(
        blocks, SPAN, heads, head_size
    )
    write_heads = jnp.repeat(
        write_activation.reshape(rows, groups, STATE), per_group, axis=1
    ).reshape(blocks, SPAN, heads, STATE)
    read_heads = jnp.repeat(read_act.reshape(rows, groups, STATE), per_group, axis=1).reshape(
        blocks, SPAN, heads, STATE
    )
    log_blocks = log_step.reshape(blocks, SPAN, heads)
    cumul = jnp.cumsum(log_blocks, axis=1)
    lower = jnp.tril(jnp.ones((SPAN, SPAN), dtype=bool))
    by_head = jnp.swapaxes(cumul, 1, 2)
    gaps = by_head[:, :, :, None] - by_head[:, :, None, :]
    weights = jnp.where(lower, jnp.exp(jnp.where(lower, gaps, 0.0)), 0.0)
    scores = jnp.einsum("bthn,bshn->bhts", read_heads, write_heads, precision=lax.Precision.HIGHEST)
    inner = jnp.einsum(
        "bhts,bshp->bthp", scores * weights, x_heads, precision=lax.Precision.HIGHEST
    )
    last = cumul[:, -1]
    fresh = jnp.einsum(
        "bshn,bshp->bhpn",
        write_heads * jnp.exp(last[:, None, :] - cumul)[:, :, :, None],
        x_heads,
        precision=lax.Precision.HIGHEST,
    )
    state_end, block_states = lax.scan(
        carry_step, jnp.zeros((heads, head_size, STATE), jnp.float32), (fresh, last)
    )
    logsum = jnp.sum(last, axis=0)
    block_prefix = jnp.cumsum(last, axis=0) - last
    start_decay = jnp.exp(block_prefix[:, None, :] + cumul)
    local_out = (
        inner
        + jnp.einsum("bthn,bhpn->bthp", read_heads, block_states, precision=lax.Precision.HIGHEST)
        * jnp.exp(cumul)[:, :, :, None]
    )
    value_full = jnp.concatenate([before[3, drop:], value_rows], axis=0).astype(jnp.float32)
    gate_full = jnp.concatenate([before[4, drop:], gate_rows], axis=0).astype(
        jnp.float32
    )
    glu = value_full * jax.nn.sigmoid(gate_full)
    long_mix = causal_valid(glu, long_taps)
    moments = jnp.stack([jnp.sum(long_mix, axis=1), jnp.sum(long_mix * long_mix, axis=1)])
    moments, piece, totals = exchanged(
        (
            moments,
            state_end.astype(jnp.bfloat16),
            jnp.broadcast_to(logsum[:, None], (heads, STATE)),
        ),
        ((("fs", "tp"), True), (("sp",), False), (("sp",), False)),
        1,
    )
    total_sum, total_square = moments[0], moments[1]
    mean = total_sum / C_CH
    spread = total_square / C_CH - mean * mean
    conv_out = jax.nn.silu(
        (long_mix - mean[:, None]) * lax.rsqrt(spread + eps_norm)[:, None] * conv_gain
    ).astype(jnp.bfloat16)
    piece = piece.astype(jnp.float32)
    totals = totals[:, :, 0]
    inclusive = jnp.cumsum(totals, axis=0)
    position = lax.axis_index("sp")
    prefix_log = lax.dynamic_index_in_dim(inclusive - totals, position, 0, keepdims=False)
    count = piece.shape[0]
    order = jnp.arange(count, dtype=jnp.int32)
    live = (order < position)[:, None]
    factor = jnp.where(live, jnp.exp(jnp.where(live, prefix_log[None, :] - inclusive, 0.0)), 0.0)
    entering = jnp.zeros_like(state_end) + jnp.einsum(
        "kh,khpn->hpn", factor, piece, precision=lax.Precision.HIGHEST
    )
    start_state = entering + jnp.exp(prefix_log)[:, None, None] * initial_state
    outputs = (
        local_out
        + jnp.einsum("bthn,hpn->bthp", read_heads, start_state, precision=lax.Precision.HIGHEST)
        * start_decay[:, :, :, None]
    )
    gated = outputs.reshape(rows, width_in) * jax.nn.silu(gate_z.astype(jnp.float32))
    return projected(
        conv_out, gated, jnp.sum(gated * gated, axis=1), state_gain, back_conv, back_state
    )


def solution(mesh):
    placed = (
        P("sp", None),
        P(),
        P("sp", ("fs", "tp")),
        P("sp", ("fs", "tp")),
        P("sp", ("fs", "tp")),
        P("sp", ("fs", "tp")),
        P("sp", ("fs", "tp")),
        P("sp", ("fs", "tp")),
        P(),
        P(("fs", "tp")),
        P(("fs", "tp")),
        P(("fs", "tp"), "sp"),
        P(None, ("fs", "tp")),
        P(None, ("fs", "tp")),
        P(None, ("fs", "tp")),
        P(None, ("fs", "tp")),
        P(("fs", "tp")),
        P(("fs", "tp")),
        P("sp", ("fs", "tp")),
        P("sp", ("fs", "tp")),
        P(("fs", "tp"), None, None),
    )
    return jax.shard_map(
        per_device,
        mesh=mesh,
        in_specs=placed,
        out_specs=P(("sp", "fs", "tp"), None),
        check_vma=False,
    )
```

```python
import functools

import jax
import jax.numpy as jnp
from jax import lax
from jax.experimental import pallas as pl
from jax.experimental.pallas import tpu as pltpu
from jax.sharding import PartitionSpec as P

C_CH = 1024
STATE = 128
WIDE_TAPS = 31
SHORT_TAPS = 4
SPAN = 64
D_INNER = 1024


eps_norm = 1e-06


def causal_valid(padded, taps):
    result = lax.conv_general_dilated(
        padded[None],
        taps[:, None, :],
        window_strides=(1,),
        padding="VALID",
        dimension_numbers=("NWC", "WIO", "NWC"),
        feature_group_count=taps.shape[1],
        precision=lax.Precision.HIGHEST,
    )
    return result[0]


MESH = pl.DeviceIdType.MESH
VMEM = pl.BlockSpec(memory_space=pltpu.VMEM)
VMEM_LIMIT = 56 * 1024 * 1024
EDGE = 32
PROJECTED = 6
HALO = 5
COLUMN_CHUNKS = 4


def gather_kernel(n, *refs):
    tokens, gain, steps = refs[:3]
    parts = refs[3:11]
    rows_out, step_out, back_conv, back_state, before = refs[11:16]
    normed, held, edge, send_sem, recv_sem, halo_send, halo_recv = refs[16:]
    me = lax.axis_index("sp")
    chunks = len(parts)
    has_left, has_right = me > 0, me < n - 1
    barrier = pltpu.get_barrier_semaphore()

    @pl.when(has_left)
    def _():
        pl.semaphore_signal(barrier, inc=1, device_id={"sp": me - 1}, device_id_type=MESH)

    @pl.when(has_right)
    def _():
        pl.semaphore_signal(barrier, inc=1, device_id={"sp": me + 1}, device_id_type=MESH)

    pl.semaphore_wait(barrier, jnp.minimum(me, 1) + jnp.minimum(n - 1 - me, 1))

    def link(src, chunk, block, way):
        return pltpu.make_async_remote_copy(
            src_ref=src,
            dst_ref=held.at[chunk, block],
            send_sem=send_sem.at[chunk, way],
            recv_sem=recv_sem.at[chunk, block],
            device_id={"sp": me + 1 if way == 0 else me - 1},
            device_id_type=MESH,
        )

    def send_own(chunk):
        @pl.when(has_right)
        def _():
            link(parts[chunk], chunk, me, 0).start()

        @pl.when(has_left)
        def _():
            link(parts[chunk], chunk, me, 1).start()

    def hop(d, chunk):
        for way, source, more in ((0, me - d, has_right), (1, me + d, has_left)):
            valid = (source >= 0) if way == 0 else (source < n)

            @pl.when(valid)
            def _():
                copy = link(held.at[chunk, source], chunk, source, way)
                copy.wait_recv()

                @pl.when(more)
                def _():
                    copy.wait_send()
                    copy.start()

    ahead = chunks
    for chunk in range(ahead):
        send_own(chunk)
    values = tokens[...].astype(jnp.float32)
    scale = lax.rsqrt(jnp.mean(values * values, axis=1, keepdims=True) + eps_norm)
    normed[...] = (values * scale * gain[...]).astype(jnp.bfloat16)
    step_out[...] = jnp.dot(normed[...], steps[...], preferred_element_type=jnp.float32)
    for chunk in range(chunks):
        held[chunk, me] = parts[chunk][...]
    rows = tokens.shape[0]
    width = parts[0].shape[1]
    depth = parts[0].shape[0]

    def round_of(d, carry):
        for chunk in range(chunks):
            hop(d, chunk)
        return carry

    lax.fori_loop(1, n - 1, round_of, 0)
    for chunk in range(chunks):
        hop(n - 1, chunk)
        if chunk < PROJECTED:
            whole = held[chunk].reshape(n * depth, width)
            rows_out[chunk] = jnp.dot(
                normed[...], whole, preferred_element_type=jnp.float32
            ).astype(jnp.bfloat16)
        if chunk == HALO - 1:
            edge[...] = rows_out[:HALO, rows - EDGE :, :]
        if chunk == HALO:

            @pl.when(has_right)
            def _():
                halo(edge, before, halo_send, halo_recv, me + 1).start()

    back_conv[...] = held[PROJECTED].reshape(n * depth, width)
    back_state[...] = held[PROJECTED + 1].reshape(n * depth, width)

    @pl.when(has_left)
    def _():
        halo(edge, before, halo_send, halo_recv, me + 1).wait_recv()

    @pl.when(me == 0)
    def _():
        before[...] = jnp.zeros_like(before)

    @pl.when(has_right)
    def _():
        halo(edge, before, halo_send, halo_recv, me + 1).wait_send()

    for chunk in range(chunks):

        @pl.when(has_right)
        def _():
            link(parts[chunk], chunk, me, 0).wait_send()

        @pl.when(has_left)
        def _():
            link(parts[chunk], chunk, me, 1).wait_send()


def halo(edge, before, send, recv, target):
    return pltpu.make_async_remote_copy(
        src_ref=edge,
        dst_ref=before,
        send_sem=send,
        recv_sem=recv,
        device_id={"sp": target},
        device_id_type=MESH,
    )


def gathered_rows(tokens, gain, steps, weights):
    n = lax.axis_size("sp")
    rows = tokens.shape[0]
    depth, width = weights[0].shape
    chunks = len(weights)
    bf16 = jnp.bfloat16
    return pl.pallas_call(
        functools.partial(gather_kernel, n),
        out_shape=(
            jax.ShapeDtypeStruct((PROJECTED, rows, width), bf16),
            jax.ShapeDtypeStruct((rows, steps.shape[1]), jnp.float32),
            jax.ShapeDtypeStruct((n * depth, width), bf16),
            jax.ShapeDtypeStruct((n * depth, width), bf16),
            jax.ShapeDtypeStruct((HALO, EDGE, width), bf16),
        ),
        in_specs=[VMEM] * (3 + chunks),
        out_specs=(VMEM,) * 5,
        scratch_shapes=[
            pltpu.VMEM(tokens.shape, bf16),
            pltpu.VMEM((chunks, n, depth, width), bf16),
            pltpu.VMEM((HALO, EDGE, width), bf16),
            pltpu.SemaphoreType.DMA((chunks, 2)),
            pltpu.SemaphoreType.DMA((chunks, n)),
            pltpu.SemaphoreType.DMA,
            pltpu.SemaphoreType.DMA,
        ],
        compiler_params=pltpu.CompilerParams(
            collective_id=0, has_side_effects=True, vmem_limit_bytes=VMEM_LIMIT
        ),
    )(tokens, gain[None, :], steps, *weights)


def peer_id(axes, sizes, index):
    if len(axes) == 1:
        return {axes[0]: index}
    return {axes[0]: index // sizes[1], axes[1]: index % sizes[1]}


def greet(axes, sizes, me, n):
    barrier = pltpu.get_barrier_semaphore()
    for i in range(1, n):
        pl.semaphore_signal(
            barrier,
            inc=1,
            device_id=peer_id(axes, sizes, lax.rem(me + i, n)),
            device_id_type=MESH,
        )
    pl.semaphore_wait(barrier, n - 1)


def index_of(axes, sizes):
    me = lax.axis_index(axes[0])
    return me if len(axes) == 1 else me * sizes[1] + lax.axis_index(axes[1])


def exchange_kernel(groups, *refs):
    count = len(groups)
    ins, outs, lands = refs[:count], refs[count : 2 * count], refs[2 * count : 3 * count]
    sems = refs[3 * count :]
    barrier = pltpu.get_barrier_semaphore()
    greeted = set()
    expected = 0
    for axes, sizes, n, add in groups:
        if axes in greeted:
            continue
        greeted.add(axes)
        me = index_of(axes, sizes)
        for i in range(1, n):
            pl.semaphore_signal(
                barrier,
                inc=1,
                device_id=peer_id(axes, sizes, lax.rem(me + i, n)),
                device_id_type=MESH,
            )
        expected += n - 1
    pl.semaphore_wait(barrier, expected)

    def copy(k, slot, land, target):
        axes, sizes, n, add = groups[k]
        return pltpu.make_async_remote_copy(
            src_ref=ins[k],
            dst_ref=lands[k].at[land],
            send_sem=sems[2 * k].at[slot],
            recv_sem=sems[2 * k + 1].at[land],
            device_id=peer_id(axes, sizes, target),
            device_id_type=MESH,
        )

    for k, (axes, sizes, n, add) in enumerate(groups):
        me = index_of(axes, sizes)
        for i in range(1, n):
            target = lax.rem(me + i, n)
            copy(k, target, me, target).start()
    for k, (axes, sizes, n, add) in enumerate(groups):
        me = index_of(axes, sizes)
        lands[k][me] = ins[k][...]
        for i in range(1, n):
            source = lax.rem(me + n - i, n)
            copy(k, source, source, source).wait_recv()
        if add:
            total = lands[k][0]
            for i in range(1, n):
                total = total + lands[k][i]
            outs[k][...] = total
        else:
            outs[k][...] = lands[k][...]
    for k, (axes, sizes, n, add) in enumerate(groups):
        me = index_of(axes, sizes)
        for i in range(1, n):
            target = lax.rem(me + i, n)
            copy(k, target, me, target).wait_send()


def exchanged(arrays, plans, number):
    groups, out, lands, sems = [], [], [], []
    for array, (axes, add) in zip(arrays, plans):
        sizes = tuple(lax.axis_size(a) for a in axes)
        n = 1
        for size in sizes:
            n *= size
        groups.append((axes, sizes, n, add))
        shape = (n,) + array.shape
        out.append(jax.ShapeDtypeStruct(array.shape if add else shape, array.dtype))
        lands.append(pltpu.VMEM(shape, array.dtype))
        sems += [pltpu.SemaphoreType.DMA((n,)), pltpu.SemaphoreType.DMA((n,))]
    count = len(arrays)
    return pl.pallas_call(
        functools.partial(exchange_kernel, tuple(groups)),
        out_shape=tuple(out),
        in_specs=[VMEM] * count,
        out_specs=(VMEM,) * count,
        scratch_shapes=lands + sems,
        compiler_params=pltpu.CompilerParams(
            collective_id=number, has_side_effects=True, vmem_limit_bytes=VMEM_LIMIT
        ),
    )(*arrays)


def project_kernel(sizes, conv, gated, square, gain, back_conv, back_state, out, *scratch):
    core_out, core_in, plane_out, plane_in, own = scratch[:5]
    core_send, core_recv, plane_send, plane_recv = scratch[5:9]
    state, squares, square_send, square_recv = scratch[9:]
    n_fs, n_tp = sizes
    fs, tp = lax.axis_index("fs"), lax.axis_index("tp")
    me = fs * n_tp + tp
    n = n_fs * n_tp
    greet(("fs", "tp"), sizes, me, n)

    def square_copy(slot, land, target):
        return pltpu.make_async_remote_copy(
            src_ref=square,
            dst_ref=squares.at[land],
            send_sem=square_send.at[slot],
            recv_sem=square_recv.at[land],
            device_id=peer_id(("fs", "tp"), sizes, target),
            device_id_type=MESH,
        )

    for i in range(1, n):
        target = lax.rem(me + i, n)
        square_copy(target, me, target).start()
    squares[me] = square[...]
    for i in range(1, n):
        source = lax.rem(me + n - i, n)
        square_copy(source, source, source).wait_recv()
    whole = squares[0]
    for i in range(1, n):
        whole = whole + squares[i]
    factor = lax.rsqrt(whole / D_INNER + eps_norm)
    factor = jnp.broadcast_to(factor, (8, factor.shape[1])).T[:, :1]
    rows = conv.shape[2]
    for f in range(n_fs):
        for c in range(n_tp):
            at = (f * n_tp + c) * rows
            state[f, c] = (gated[f, c] * factor[at : at + rows] * gain[...]).astype(jnp.bfloat16)
    block = conv.shape[2]
    wide = back_conv.shape[0] // COLUMN_CHUNKS
    contract = (((1,), (1,)), ((), ()))

    def term(core, j):
        left = jnp.concatenate([conv[f, core] for f in range(n_fs)], axis=0)
        right = jnp.concatenate([state[f, core] for f in range(n_fs)], axis=0)
        at = pl.ds(j * wide, wide)
        return lax.dot_general(
            left, back_conv[at, :], contract, preferred_element_type=jnp.float32
        ) + lax.dot_general(
            right, back_state[at, :], contract, preferred_element_type=jnp.float32
        )

    def core_copy(step, j):
        target = lax.rem(tp + step, n_tp)
        return pltpu.make_async_remote_copy(
            src_ref=core_out.at[step - 1, j],
            dst_ref=core_in.at[step - 1, j],
            send_sem=core_send.at[step - 1, j],
            recv_sem=core_recv.at[step - 1, j],
            device_id={"tp": target},
            device_id_type=MESH,
        )

    def plane_copy(step, j):
        target = lax.rem(fs + step, n_fs)
        return pltpu.make_async_remote_copy(
            src_ref=plane_out.at[target, j],
            dst_ref=plane_in.at[step - 1, j],
            send_sem=plane_send.at[step - 1, j],
            recv_sem=plane_recv.at[step - 1, j],
            device_id={"fs": target},
            device_id_type=MESH,
        )

    def send_core(j):
        for step in range(1, n_tp):
            core_copy(step, j).start()

    def send_plane(j):
        for step in range(1, n_fs):
            plane_copy(step, j).start()

    for j in range(COLUMN_CHUNKS):
        for step in range(1, n_tp):
            core_out[step - 1, j] = term(lax.rem(tp + step, n_tp), j).astype(jnp.bfloat16)
        if j:
            send_core(j - 1)
    mine = term(tp, 0)
    send_core(COLUMN_CHUNKS - 1)
    for j in range(COLUMN_CHUNKS):
        total = mine
        for step in range(1, n_tp):
            core_copy(step, j).wait_recv()
            total = total + core_in[step - 1, j].astype(jnp.float32)
        for f in range(n_fs):
            part = total[f * block : (f + 1) * block]
            plane_out[f, j] = part.astype(jnp.bfloat16)

            @pl.when(f == fs)
            def _():
                own[j] = part

        if j + 1 < COLUMN_CHUNKS:
            mine = term(tp, j + 1)
        send_plane(j)
    for j in range(COLUMN_CHUNKS):
        total = own[j]
        for step in range(1, n_fs):
            plane_copy(step, j).wait_recv()
            total = total + plane_in[step - 1, j].astype(jnp.float32)
        out[:, j * wide : (j + 1) * wide] = total.astype(jnp.bfloat16)
    for i in range(1, n):
        target = lax.rem(me + i, n)
        square_copy(target, me, target).wait_send()
    for j in range(COLUMN_CHUNKS):
        for step in range(1, n_tp):
            core_copy(step, j).wait_send()
        for step in range(1, n_fs):
            plane_copy(step, j).wait_send()


def projected(conv, gated, square, gain, back_conv, back_state):
    n_fs, n_tp = sizes = (lax.axis_size("fs"), lax.axis_size("tp"))
    rows, width = conv.shape
    block = rows // (n_fs * n_tp)
    features = back_conv.shape[0]
    wide = features // COLUMN_CHUNKS
    k = COLUMN_CHUNKS
    bf16 = jnp.bfloat16
    shaped = (n_fs, n_tp, block, width)
    return pl.pallas_call(
        functools.partial(project_kernel, sizes),
        out_shape=jax.ShapeDtypeStruct((block, features), bf16),
        in_specs=[VMEM] * 6,
        out_specs=VMEM,
        scratch_shapes=[
            pltpu.VMEM((n_tp - 1, k, n_fs * block, wide), bf16),
            pltpu.VMEM((n_tp - 1, k, n_fs * block, wide), bf16),
            pltpu.VMEM((n_fs, k, block, wide), bf16),
            pltpu.VMEM((n_fs - 1, k, block, wide), bf16),
            pltpu.VMEM((k, block, wide), jnp.float32),
            pltpu.SemaphoreType.DMA((n_tp - 1, k)),
            pltpu.SemaphoreType.DMA((n_tp - 1, k)),
            pltpu.SemaphoreType.DMA((n_fs - 1, k)),
            pltpu.SemaphoreType.DMA((n_fs - 1, k)),
            pltpu.VMEM(shaped, bf16),
            pltpu.VMEM((n_fs * n_tp, 1, rows), jnp.float32),
            pltpu.SemaphoreType.DMA((n_fs * n_tp,)),
            pltpu.SemaphoreType.DMA((n_fs * n_tp,)),
        ],
        compiler_params=pltpu.CompilerParams(
            collective_id=4, has_side_effects=True, vmem_limit_bytes=VMEM_LIMIT
        ),
    )(
        conv.reshape(shaped),
        gated.reshape(shaped),
        square[None, :],
        gain[None, :],
        back_conv,
        back_state,
    )


def carry_step(state, inputs):
    fresh, last = inputs
    return (state * jnp.exp(last)[:, None, None] + fresh, state)


def per_device(
    tokens,
    norm_gain,
    conv_value,
    conv_gate,
    mixer_gate,
    state_input,
    write_projection,
    state_read,
    step_proj,
    step_bias,
    decay_log,
    decay_extra,
    input_taps,
    write_taps,
    fetch_kernel_coefficients,
    long_taps,
    conv_gain,
    state_gain,
    conv_output,
    state_output,
    initial_state,
):
    rows = tokens.shape[0]
    channels = conv_value.shape[1]
    width_in = state_input.shape[1]
    width_group = write_projection.shape[1]
    heads = step_bias.shape[0]
    groups = width_group // STATE
    per_group = heads // groups
    head_size = width_in // heads
    projected_rows, step_all, back_conv, back_state, before = gathered_rows(
        tokens,
        norm_gain,
        step_proj,
        (
            state_input,
            write_projection,
            state_read,
            conv_value,
            conv_gate,
            mixer_gate,
            conv_output,
            state_output,
        ),
    )
    input_rows, write_rows, read_rows, value_rows, gate_rows, gate_z = (
        projected_rows[i] for i in range(PROJECTED)
    )
    head_start = (lax.axis_index("fs") * lax.axis_size("tp") + lax.axis_index("tp")) * heads
    step_raw = lax.dynamic_slice_in_dim(step_all, head_start, heads, 1)
    step_size = jax.nn.softplus(step_raw + step_bias)
    log_step = -jnp.exp(decay_log) * step_size + decay_extra.T
    drop = EDGE - WIDE_TAPS + 1
    short_edge = jnp.concatenate(
        [before[i, EDGE - SHORT_TAPS + 1 :] for i in range(3)], axis=1
    )
    state_row_values = jnp.concatenate([input_rows, write_rows, read_rows], axis=1)
    state_full = jnp.concatenate([short_edge, state_row_values], axis=0).astype(jnp.float32)
    state_taps = jnp.concatenate([input_taps, write_taps, fetch_kernel_coefficients], axis=1)
    activated = jax.nn.silu(causal_valid(state_full, state_taps))
    input_act = activated[:, :width_in]
    write_activation = activated[:, width_in : width_in + width_group]
    read_act = activated[:, width_in + width_group :]
    blocks = rows // SPAN
    x_heads = (input_act.reshape(rows, heads, head_size) * step_size[:, :, None]).reshape(
        blocks, SPAN, heads, head_size
    )
    write_heads = jnp.repeat(
        write_activation.reshape(rows, groups, STATE), per_group, axis=1
    ).reshape(blocks, SPAN, heads, STATE)
    read_heads = jnp.repeat(read_act.reshape(rows, groups, STATE), per_group, axis=1).reshape(
        blocks, SPAN, heads, STATE
    )
    log_blocks = log_step.reshape(blocks, SPAN, heads)
    cumul = jnp.cumsum(log_blocks, axis=1)
    lower = jnp.tril(jnp.ones((SPAN, SPAN), dtype=bool))
    by_head = jnp.swapaxes(cumul, 1, 2)
    gaps = by_head[:, :, :, None] - by_head[:, :, None, :]
    weights = jnp.where(lower, jnp.exp(jnp.where(lower, gaps, 0.0)), 0.0)
    scores = jnp.einsum("bthn,bshn->bhts", read_heads, write_heads, precision=lax.Precision.HIGHEST)
    inner = jnp.einsum(
        "bhts,bshp->bthp", scores * weights, x_heads, precision=lax.Precision.HIGHEST
    )
    last = cumul[:, -1]
    fresh = jnp.einsum(
        "bshn,bshp->bhpn",
        write_heads * jnp.exp(last[:, None, :] - cumul)[:, :, :, None],
        x_heads,
        precision=lax.Precision.HIGHEST,
    )
    state_end, block_states = lax.scan(
        carry_step, jnp.zeros((heads, head_size, STATE), jnp.float32), (fresh, last)
    )
    logsum = jnp.sum(last, axis=0)
    block_prefix = jnp.cumsum(last, axis=0) - last
    start_decay = jnp.exp(block_prefix[:, None, :] + cumul)
    local_out = (
        inner
        + jnp.einsum("bthn,bhpn->bthp", read_heads, block_states, precision=lax.Precision.HIGHEST)
        * jnp.exp(cumul)[:, :, :, None]
    )
    value_full = jnp.concatenate([before[3, drop:], value_rows], axis=0).astype(jnp.float32)
    gate_full = jnp.concatenate([before[4, drop:], gate_rows], axis=0).astype(
        jnp.float32
    )
    glu = value_full * jax.nn.sigmoid(gate_full)
    long_mix = causal_valid(glu, long_taps)
    moments = jnp.stack([jnp.sum(long_mix, axis=1), jnp.sum(long_mix * long_mix, axis=1)])
    moments, piece, totals = exchanged(
        (
            moments,
            state_end.astype(jnp.bfloat16),
            jnp.broadcast_to(logsum[:, None], (heads, STATE)),
        ),
        ((("fs", "tp"), True), (("sp",), False), (("sp",), False)),
        1,
    )
    total_sum, total_square = moments[0], moments[1]
    mean = total_sum / C_CH
    spread = total_square / C_CH - mean * mean
    conv_out = jax.nn.silu(
        (long_mix - mean[:, None]) * lax.rsqrt(spread + eps_norm)[:, None] * conv_gain
    ).astype(jnp.bfloat16)
    piece = piece.astype(jnp.float32)
    totals = totals[:, :, 0]
    inclusive = jnp.cumsum(totals, axis=0)
    position = lax.axis_index("sp")
    prefix_log = lax.dynamic_index_in_dim(inclusive - totals, position, 0, keepdims=False)
    count = piece.shape[0]
    order = jnp.arange(count, dtype=jnp.int32)
    live = (order < position)[:, None]
    factor = jnp.where(live, jnp.exp(jnp.where(live, prefix_log[None, :] - inclusive, 0.0)), 0.0)
    entering = jnp.zeros_like(state_end) + jnp.einsum(
        "kh,khpn->hpn", factor, piece, precision=lax.Precision.HIGHEST
    )
    start_state = entering + jnp.exp(prefix_log)[:, None, None] * initial_state
    outputs = (
        local_out
        + jnp.einsum("bthn,hpn->bthp", read_heads, start_state, precision=lax.Precision.HIGHEST)
        * start_decay[:, :, :, None]
    )
    gated = outputs.reshape(rows, width_in) * jax.nn.silu(gate_z.astype(jnp.float32))
    return projected(
        conv_out, gated, jnp.sum(gated * gated, axis=1), state_gain, back_conv, back_state
    )


def solution(mesh):
    placed = (
        P("sp", None),
        P(),
        P("sp", ("fs", "tp")),
        P("sp", ("fs", "tp")),
        P("sp", ("fs", "tp")),
        P("sp", ("fs", "tp")),
        P("sp", ("fs", "tp")),
        P("sp", ("fs", "tp")),
        P(),
        P(("fs", "tp")),
        P(("fs", "tp")),
        P(("fs", "tp"), "sp"),
        P(None, ("fs", "tp")),
        P(None, ("fs", "tp")),
        P(None, ("fs", "tp")),
        P(None, ("fs", "tp")),
        P(("fs", "tp")),
        P(("fs", "tp")),
        P("sp", ("fs", "tp")),
        P("sp", ("fs", "tp")),
        P(("fs", "tp"), None, None),
    )
    return jax.shard_map(
        per_device,
        mesh=mesh,
        in_specs=placed,
        out_specs=P(("sp", "fs", "tp"), None),
        check_vma=False,
    )
```
